32 devices in a mesh: sp: 16 (over z, y, x), tp: 2 (over core).
Axes of the slice: x: 2, y: 2, z: 4, core: 2. Of those that a mesh axis runs over, the one named last changes fastest.
Arguments:
- query: bfloat16 [2048, 2048], P('sp', 'tp'), may hold values from -6 to 6
- forget_logit: bfloat16 [2048, 2048], P('sp', 'tp'), may hold values from -7.5 to 7.5
- value: bfloat16 [2048, 2048], P('sp', 'tp'), may hold values from -6 to 6
- out_gate: bfloat16 [2048, 2048], P('sp', 'tp'), may hold values from -6 to 6
- lower_bound: float32 [2048], P('tp'), may hold values from 0.9 to 1, as said below
- head_gain: float32 [2048], P('tp'), may hold values from 0.1 to 1.9
- residual_in: bfloat16 [2048, 2048], P(('sp', 'tp')), may hold values from -6 to 6
- w_out: bfloat16 [2048, 2048], replicated, may hold values from -0.125 to 0.125
- ffn_gain: float32 [2048], replicated, may hold values from 0.1 to 1.9
- routing: int32 [2048, 2], P(('sp', 'tp')), may hold values from 0 to 15, all different within a row; in each aligned block of 64 rows (0 to 63, 64 to 127, ...) at most 16 rows name the same one
- route_weight: float32 [2048, 2], P(('sp', 'tp')), may hold values from 0.25 to 1
- expert_gate: bfloat16 [16, 2048, 1024], P('sp', None, 'tp'), may hold values from -0.125 to 0.125
- expert_up: bfloat16 [16, 2048, 1024], P('sp', None, 'tp'), may hold values from -0.125 to 0.125
- expert_down: bfloat16 [16, 1024, 2048], P('sp', 'tp'), may hold values from -0.1875 to 0.1875
Outputs:
- layer_out: bfloat16 [2048, 2048], P(('sp', 'tp'))
The draws below stay inside these ranges and needn't reach their ends.
Inputs may be any that keep to these rules, and one draw needn't show every extreme that they name: `routing`: each row names 2 different experts. In each aligned block of 64 rows (the rows of one device) no expert is named by more than 16 rows, a bound that some blocks reach. 1 - lower_bound is at least 1 / 4096.
All inputs are finite; a program needn't handle non-finite values.
Results may differ from the reference program's by a relative error of at most 0.012.
Values may be sent and summed in bfloat16 or wider, within the bound.
A program may use at most 128 MiB of HBM per device.

```python
import math
import jax
import jax.numpy as jnp
import numpy as np
from jax import lax

D = 2048
HEADS = 16
HEAD_DIM = 128
FF = 1024
TOP_K = 2
BLOCK = 16
TOKENS = 2048
HALF = 64
EXPERTS = 16
CAP = 16
N_SP = 16
N_TP = 2


def draw_lower_bound(key, part):
    order_key, slow_key, fast_key, middle_key = jax.random.split(jax.random.fold_in(key, 11), 4)
    slow_count = HEADS // 2
    middle_count = max(1, HEADS // 5)
    ranks = jax.random.permutation(order_key, HEADS)
    middle_heads = ranks < middle_count
    slow_heads = ranks < slow_count
    slow_gap = jnp.exp(jax.random.uniform(slow_key, (HEADS, HEAD_DIM), jnp.float32, jnp.log(0.5), jnp.log(3.0))) / TOKENS
    fast_gap = jnp.exp(jax.random.uniform(fast_key, (HEADS, HEAD_DIM), jnp.float32, jnp.log(0.03), jnp.log(0.1)))
    middle_gap = jnp.exp(jax.random.uniform(middle_key, (HEADS, HEAD_DIM), jnp.float32, jnp.log(0.002), jnp.log(0.008)))
    gap_values = jnp.where(slow_heads[:, None], slow_gap, fast_gap)
    gap_values = jnp.where(middle_heads[:, None], middle_gap, gap_values)
    return (1.0 - gap_values).reshape(-1).astype(jnp.float32)


def draw_forget_logit(key, part):
    rough_key, span_key, wide_key = jax.random.split(jax.random.fold_in(key, 23), 3)
    width = HEADS * HEAD_DIM
    rows = jnp.arange(TOKENS)
    rough = jax.random.normal(rough_key, (TOKENS, width), jnp.float32)
    offsets = jax.random.uniform(span_key, (TOKENS // 128 + 1, width), jnp.float32, -1.5, 1.5)
    wide = jax.random.uniform(wide_key, (TOKENS // 1024 + 1, HEADS), jnp.float32, -1.5, 6.0)
    wide_full = jnp.repeat(wide, HEAD_DIM, axis=1)
    values = rough + offsets[rows // 128] + wide_full[rows // 1024]
    return jnp.clip(values, -7.5, 7.5).astype(jnp.bfloat16)


def block_scale(rng, extent, shards, low, top_value):
    loudness = 1.0
    for dim, parts in shards:
        steps = jax.random.uniform(jax.random.fold_in(jax.random.fold_in(rng, 6), dim), (parts,), jnp.float32, low / len(shards), top_value / len(shards))
        loudness = loudness * jnp.repeat(jnp.exp(steps), extent[dim] // parts).reshape((-1,) + (1,) * (len(extent) - 1 - dim))
    return loudness


def routed_block(key, own, number, rows, number_of, top, most, skew):
    order = jax.random.permutation(key, number_of)
    heavy_load, usual = load_shares(number_of, rows * top, most, skew, True), load_shares(number_of, rows * top, most, skew, False)
    places = jnp.arange(number_of)

    def named(sizes, rotation):
        used = int((sizes > 0).sum())
        fixed = max(1, used // 4)
        shifted = fixed + (places - fixed + rotation * (used - fixed)) % max(1, number_of - fixed)
        return jnp.zeros((number_of,), jnp.int32).at[order[jnp.where(places < fixed, places, shifted)]].set(jnp.asarray(sizes, jnp.int32))

    sizes = jnp.where(number % 4 == 0, named(heavy_load, number // 4), named(usual, number - number // 4 - 1))
    mixed = jax.random.permutation(jax.random.fold_in(own, 3), number_of)
    donor, taker = mixed[0:number_of // 2 * 2:2], mixed[1:number_of // 2 * 2:2]
    room = jnp.minimum(sizes[donor] - 1, most - sizes[taker]) // 2
    room = jnp.where((donor == order[0]) | (taker == order[0]) | (sizes[taker] == 0), 0, jnp.maximum(room, 0))
    shifted = jax.random.randint(jax.random.fold_in(own, 4), (number_of // 2,), 0, 1 << 20) % (room + 1)
    sizes = sizes.at[donor].add(-shifted).at[taker].add(shifted)
    labels = jnp.searchsorted(jnp.cumsum(sizes), jnp.arange(rows * top), side="right").astype(jnp.int32)
    table = labels.reshape(top, rows).T
    table = table[jax.random.permutation(jax.random.fold_in(own, 1), rows)]
    rotation = jax.random.randint(jax.random.fold_in(own, 2), (rows, 1), 0, top)
    return jnp.take_along_axis(table, (jnp.arange(top)[None, :] + rotation) % top, axis=1)


def load_shares(count, total, bound, slope, full):
    weights = [(1 << 20) // math.isqrt(rank ** slope) + 1 for rank in range(1, count + 1)]
    largest = bound if full else min(bound, max(-(-total // count), total * weights[0] // sum(weights)))
    least = 1 if total - largest >= count - 1 else 0
    holding, surplus = [largest] + [least] * (count - 1), total - largest - least * (count - 1)
    while surplus > 0:
        free = [i for i in range(1, count) if holding[i] < largest] or [i for i in range(1, count) if holding[i] < bound]
        pool, left = sum([weights[i] for i in free]), surplus
        for i in free:
            more = min(bound - holding[i], max(1, left * weights[i] // pool), surplus)
            holding[i] = holding[i] + more
            surplus = surplus - more
    return np.array(holding)


def scatter_about(stream_key, shape, deviation, bound, cuts=(), kind=jnp.bfloat16):
    values = deviation * jax.random.normal(stream_key, shape, jnp.float32)
    if cuts:
        values = values * block_scale(stream_key, shape, cuts, -0.22, 0.18)
    return jnp.clip(values, -bound, bound).astype(kind)


def setup_inputs(seed: int = 0) -> dict:
    arg_keys = jax.random.split(jax.random.key(seed), 15)
    query = scatter_about(arg_keys[0], (TOKENS, HEADS * HEAD_DIM), 1.0, 6.0, ((0, 16), (1, 2)))
    forget_logit = draw_forget_logit(jax.random.fold_in(arg_keys[14], 71), 0)
    value = scatter_about(arg_keys[2], (TOKENS, HEADS * HEAD_DIM), 1.0, 6.0, ((0, 16), (1, 2)))
    out_gate = scatter_about(arg_keys[3], (TOKENS, HEADS * HEAD_DIM), 1.0, 6.0, ((0, 16), (1, 2)))
    lower_bound = draw_lower_bound(jax.random.fold_in(arg_keys[14], 71), 0)
    head_gain = jnp.clip(1.0 + 0.18 * jax.random.normal(arg_keys[5], (HEADS * HEAD_DIM,), jnp.float32), 0.1, 1.9)
    residual_in = scatter_about(arg_keys[6], (TOKENS, D), 1.0, 6.0, ((0, 32),))
    w_out = scatter_about(arg_keys[7], (HEADS * HEAD_DIM, D), (HEADS * HEAD_DIM) ** -0.5, 0.125)
    ffn_gain = jnp.clip(1.0 + 0.18 * jax.random.normal(arg_keys[8], (D,), jnp.float32), 0.1, 1.9)
    routing_keys = jax.random.split(jax.random.fold_in(arg_keys[9], 1), TOKENS // HALF)
    routing_turns = jax.random.permutation(jax.random.fold_in(arg_keys[9], 3), TOKENS // HALF)
    routing = jax.vmap(lambda own, number: routed_block(jax.random.fold_in(arg_keys[9], 2), own, number, HALF, EXPERTS, TOP_K, CAP, 2))(routing_keys, routing_turns).reshape((TOKENS, TOP_K))
    route_weight = jnp.clip(0.25 + 0.75 * jax.random.uniform(arg_keys[10], (TOKENS, TOP_K), jnp.float32) ** block_scale(arg_keys[10], (TOKENS, TOP_K), ((0, 32),), -0.2, 0.2), 0.25, 1.0)
    expert_gate = scatter_about(arg_keys[11], (EXPERTS, D, FF), D ** -0.5, 0.125, ((0, 16), (2, 2)))
    expert_up = scatter_about(arg_keys[12], (EXPERTS, D, FF), D ** -0.5, 0.125, ((0, 16), (2, 2)))
    expert_down = scatter_about(arg_keys[13], (EXPERTS, FF, D), FF ** -0.5, 0.1875, ((0, 16), (1, 2)))
    return {"query": query, "forget_logit": forget_logit, "value": value, "out_gate": out_gate, "lower_bound": lower_bound, "head_gain": head_gain, "residual_in": residual_in, "w_out": w_out, "ffn_gain": ffn_gain, "routing": routing, "route_weight": route_weight, "expert_gate": expert_gate, "expert_up": expert_up, "expert_down": expert_down}


epsilon = 1e-06
highest = lax.Precision.HIGHEST

def recurrence(queries, log_forget, key_gate, values):
    blocks = queries.shape[0] // BLOCK

    def to_blocks(table):
        return table.reshape(blocks, BLOCK, HEADS, HEAD_DIM)
    causal = jnp.arange(BLOCK)[:, None] >= jnp.arange(BLOCK)[None, :]

    def advance(state, inputs):
        query_b, forget_b, key_b, value_b = inputs
        cumulative = jnp.cumsum(forget_b, axis=0)
        log_gaps = cumulative[:, None] - cumulative[None, :]
        decays = jnp.exp(jnp.where(causal[:, :, None, None], log_gaps, -jnp.inf))
        scores = jnp.einsum('thd,shd,tshd->hts', query_b, key_b, decays, precision=highest)
        result = jnp.einsum('hts,shv->thv', scores, value_b, precision=highest)
        result = result + jnp.einsum('thd,hdv->thv', query_b * jnp.exp(cumulative), state, precision=highest)
        last_log = cumulative[-1]
        weighted = key_b * jnp.exp(last_log[None] - cumulative)
        state = jnp.exp(last_log)[:, :, None] * state + jnp.einsum('shd,shv->hdv', weighted, value_b, precision=highest)
        return (state, result)
    initial = jnp.zeros((HEADS, HEAD_DIM, HEAD_DIM), jnp.float32)
    _, head_out = lax.scan(advance, initial, (to_blocks(queries), to_blocks(log_forget), to_blocks(key_gate), to_blocks(values)))
    return head_out.reshape(-1, HEADS, HEAD_DIM)

def expert_pass(normed, routing, route_weight, expert_gate, expert_up, expert_down):
    flat_routes = routing.reshape(-1)
    flat_weights = route_weight.reshape(-1)
    most_rows = N_SP * N_TP * CAP

    def visit(running, inputs):
        expert_id, gate_w, up_w, down_w = inputs
        matches = flat_routes == expert_id
        slots_found = jnp.nonzero(matches, size=most_rows, fill_value=0)[0]
        filled = jnp.arange(most_rows) < jnp.sum(matches)
        owners = slots_found // TOP_K
        taken = normed[owners]
        gate_part = jnp.dot(taken, gate_w, preferred_element_type=jnp.float32)
        up_part = jnp.dot(taken, up_w, preferred_element_type=jnp.float32)
        hidden = (jax.nn.silu(gate_part) * up_part).astype(jnp.bfloat16)
        expert_out = jnp.dot(hidden, down_w, preferred_element_type=jnp.float32).astype(jnp.bfloat16)
        scaled = jnp.where(filled, flat_weights[slots_found], 0.0)
        running = running.at[owners].add(expert_out.astype(jnp.float32) * scaled[:, None])
        return (running, None)
    initial = jnp.zeros(normed.shape, jnp.float32)
    expert_ids = jnp.arange(EXPERTS, dtype=jnp.int32)
    summed, _ = lax.scan(visit, initial, (expert_ids, expert_gate, expert_up, expert_down))
    return summed

def reference(query, forget_logit, value, out_gate, lower_bound, head_gain, residual_in, w_out, ffn_gain, routing, route_weight, expert_gate, expert_up, expert_down):
    positions = query.shape[0]
    grid = (positions, HEADS, HEAD_DIM)
    floor_gate = lower_bound.reshape(HEADS, HEAD_DIM)
    logits = forget_logit.astype(jnp.float32).reshape(grid)
    log_forget = jnp.logaddexp(jnp.log(floor_gate), jnp.log1p(-floor_gate) + jax.nn.log_sigmoid(logits))
    key_gate = (1.0 - floor_gate) * jax.nn.sigmoid(-logits)
    head_out = recurrence(query.astype(jnp.float32).reshape(grid), log_forget, key_gate, value.astype(jnp.float32).reshape(grid))
    normed_heads = head_out * lax.rsqrt(lax.optimization_barrier(jnp.mean(head_out * head_out, axis=-1, keepdims=True)) + epsilon)
    gates = jax.nn.silu(out_gate.astype(jnp.float32).reshape(grid))
    mixed = (normed_heads * head_gain.reshape(HEADS, HEAD_DIM) * gates).astype(jnp.bfloat16).reshape(positions, -1)
    projected = jnp.dot(mixed, w_out, preferred_element_type=jnp.float32)
    updated = (residual_in.astype(jnp.float32) + projected).astype(jnp.bfloat16)
    updated_f = updated.astype(jnp.float32)
    normed = (updated_f * lax.rsqrt(lax.optimization_barrier(jnp.mean(updated_f * updated_f, axis=-1, keepdims=True)) + epsilon) * ffn_gain).astype(jnp.bfloat16)
    expert_sum = expert_pass(normed, routing, route_weight, expert_gate, expert_up, expert_down)
    return (updated_f + expert_sum).astype(jnp.bfloat16)
```

```python
import functools

import jax
import jax.numpy as jnp
from jax import lax
from jax.experimental import pallas as pl
from jax.experimental.pallas import tpu as pltpu
from jax.sharding import PartitionSpec as P

HEAD_DIM = 128
MESH = pl.DeviceIdType.MESH
epsilon = 1e-06
f32 = jnp.float32
bf16 = jnp.bfloat16
NT = (((1,), (1,)), ((), ()))
TN = (((0,), (0,)), ((), ()))


def dot(a, b, dims=(((1,), (0,)), ((), ())), precision=None):
    return lax.dot_general(a, b, dims, precision=precision, preferred_element_type=f32)


def rows_of(index, count):
    return pl.ds(pl.multiple_of(index * count, count), count)


def greet(n):
    me, core = lax.axis_index("sp"), lax.axis_index("tp")
    barrier = pltpu.get_barrier_semaphore()
    pl.semaphore_signal(barrier, inc=1, device_id={"tp": 1 - core}, device_id_type=MESH)

    @pl.loop(1, n)
    def _(r):
        pl.semaphore_signal(
            barrier, inc=1, device_id={"sp": lax.rem(me + r, n)}, device_id_type=MESH
        )

    return barrier


def scan_kernel(
    n, cap,
    query, logit, value, gate, bound, gain, residual, ffn_gain, routing, weight, w_hbm,
    updated_out, outbox_out, combine_out,
    w_out, q_scr, k_scr, ho, st_send, st_recv, dec_send, dec_recv, ret_send, ret_recv,
    mixed, regrouped, proj, w_sem, s_sem, r_sem, ds_sem, dr_sem, bs_sem, br_sem, ms_sem, mr_sem,
):
    me, core = lax.axis_index("sp"), lax.axis_index("tp")
    length, width = query.shape
    heads = width // HEAD_DIM
    piece = width // n
    half = length // 2
    w_copy = pltpu.make_async_copy(w_hbm, w_out, w_sem)
    w_copy.start()
    barrier = greet(n)

    row = lax.broadcasted_iota(jnp.int32, (length, length), 0)
    col = lax.broadcasted_iota(jnp.int32, (length, length), 1)
    causal = row >= col
    tri = causal.astype(f32)
    for h in range(heads):
        c = slice(h * HEAD_DIM, (h + 1) * HEAD_DIM)
        key = (1.0 - bound[:, c]) / (1.0 + jnp.exp(logit[:, c].astype(f32)))
        cum = dot(tri, jnp.log1p(-key), precision=lax.Precision.HIGHEST)
        last = cum[length - 1 :, :]
        mid = 0.5 * last
        q_scr[:, c] = (query[:, c].astype(f32) * jnp.exp(cum - mid)).astype(bf16)
        keys = (key * jnp.exp(mid - cum)).astype(bf16)
        k_scr[:, c] = keys
        st_send[c, :] = (dot(value[:, c], keys, TN) * jnp.exp(mid)).astype(bf16)
        dec_send[h : h + 1, :] = last

    def state_copy(dst, src):
        return pltpu.make_async_remote_copy(
            src_ref=st_send.at[rows_of(dst, piece)], dst_ref=st_recv.at[src],
            send_sem=s_sem.at[dst], recv_sem=r_sem.at[src],
            device_id={"sp": dst}, device_id_type=MESH,
        )

    def decay_copy(dst, src):
        return pltpu.make_async_remote_copy(
            src_ref=dec_send, dst_ref=dec_recv.at[src],
            send_sem=ds_sem.at[dst], recv_sem=dr_sem.at[src],
            device_id={"sp": dst}, device_id_type=MESH,
        )

    def back_copy(dst, src):
        return pltpu.make_async_remote_copy(
            src_ref=ret_send.at[dst], dst_ref=ret_recv.at[rows_of(src, piece)],
            send_sem=bs_sem.at[dst], recv_sem=br_sem.at[src],
            device_id={"sp": dst}, device_id_type=MESH,
        )

    pl.semaphore_wait(barrier, n)

    @pl.loop(1, n)
    def _(r):
        dst = lax.rem(me + r, n)
        decay_copy(dst, me).start()
        state_copy(dst, me).start()

    st_recv[me] = st_send[rows_of(me, piece), :]
    dec_recv[me] = dec_send[...]

    for h in range(heads):
        c = slice(h * HEAD_DIM, (h + 1) * HEAD_DIM)
        scores = jnp.where(causal, dot(q_scr[:, c], k_scr[:, c], NT), 0.0).astype(bf16)
        ho[:, c] = dot(scores, value[:, c])

    slots = n * cap
    count = routing.shape[0]
    expert = lax.broadcasted_iota(jnp.int32, (count, n), 1)
    slot_of = lax.broadcasted_iota(jnp.int32, (count, slots), 1)
    before = (
        lax.broadcasted_iota(jnp.int32, (count, count), 0)
        > lax.broadcasted_iota(jnp.int32, (count, count), 1)
    ).astype(bf16)
    used = jnp.zeros((1, n), f32)
    picks = jnp.zeros((count, slots), f32)
    combine = jnp.zeros((count, slots), f32)
    for k in range(routing.shape[1]):
        hot = (routing[:, k : k + 1] == expert).astype(f32)
        rank = dot(before, hot.astype(bf16)) + used
        used = used + jnp.sum(hot, axis=0, keepdims=True)
        slot = jnp.sum(hot * (rank + expert.astype(f32) * cap), axis=1, keepdims=True)
        mine = slot.astype(jnp.int32) == slot_of
        picks = jnp.where(mine, 1.0, picks)
        combine = jnp.where(mine, weight[:, k : k + 1], combine)
    combine_out[...] = combine

    @pl.loop(1, n)
    def _(r):
        src = lax.rem(me + r, n)
        decay_copy(me, src).wait_recv()
        state_copy(me, src).wait_recv()

    my_head = me * piece // HEAD_DIM

    def prefix(p, acc):
        last = dec_recv[p, pl.ds(my_head, 1), :]
        ret_send[p] = (acc * jnp.exp(0.5 * last)).astype(bf16)
        return acc * jnp.exp(last) + st_recv[p].astype(f32)

    lax.fori_loop(0, n, prefix, jnp.zeros((piece, HEAD_DIM), f32))

    @pl.loop(1, n)
    def _(r):
        back_copy(lax.rem(me + r, n), me).start()

    ret_recv[rows_of(me, piece), :] = ret_send[me]

    @pl.loop(1, n)
    def _(r):
        back_copy(me, lax.rem(me + r, n)).wait_recv()

    for h in range(heads):
        c = slice(h * HEAD_DIM, (h + 1) * HEAD_DIM)
        out = ho[:, c] + dot(q_scr[:, c], ret_recv[c, :], NT)
        out = out * lax.rsqrt(jnp.mean(out * out, axis=1, keepdims=True) + epsilon)
        g = gate[:, c].astype(f32)
        out = (out * gain[:, c] * (g / (1.0 + jnp.exp(-g)))).astype(bf16)
        mixed[0, :, c] = out[:half]
        mixed[1, :, c] = out[half:]

    swap = pltpu.make_async_remote_copy(
        src_ref=mixed.at[1 - core], dst_ref=regrouped,
        send_sem=ms_sem, recv_sem=mr_sem,
        device_id={"tp": 1 - core}, device_id_type=MESH,
    )
    swap.start()
    w_copy.wait()
    tile = 512
    total = w_out.shape[1]

    def project(which, source, first):
        @pl.loop(0, total // tile)
        def _(j):
            cols = pl.ds(pl.multiple_of(j * tile, tile), tile)
            part = dot(source, w_out[rows_of(which, width), cols])
            proj[:, cols] = part if first else proj[:, cols] + part

    project(core, mixed[core], True)
    swap.wait()
    project(1 - core, regrouped[...], False)
    updated = (residual[...].astype(f32) + proj[...]).astype(bf16)
    updated_out[...] = updated
    updated = updated.astype(f32)
    normed = (
        updated
        * lax.rsqrt(jnp.mean(updated * updated, axis=1, keepdims=True) + epsilon)
        * ffn_gain[...]
    ).astype(bf16)
    outbox_out[...] = dot(picks.astype(bf16), normed, TN).astype(bf16)

    @pl.loop(1, n)
    def _(r):
        dst = lax.rem(me + r, n)
        decay_copy(dst, me).wait_send()
        state_copy(dst, me).wait_send()
        back_copy(dst, me).wait_send()


def expert_kernel(
    n, cap,
    outbox, updated, combine, g_hbm, u_hbm, d_hbm,
    out,
    wg, wu, wd, arrived, hidden, result, returned,
    l_sem, ps_sem, pr_sem, s_sem, r_sem, bs_sem, br_sem,
):
    me, core = lax.axis_index("sp"), lax.axis_index("tp")
    barrier = greet(n)
    homes = ((g_hbm, wg), (u_hbm, wu), (d_hbm, wd))
    local = [
        pltpu.make_async_copy(src.at[0], dst.at[0], l_sem.at[i])
        for i, (src, dst) in enumerate(homes)
    ]
    for copy in local:
        copy.start()

    def send_copy(dst, src):
        return pltpu.make_async_remote_copy(
            src_ref=outbox.at[rows_of(dst, cap)], dst_ref=arrived.at[rows_of(src, cap)],
            send_sem=s_sem.at[dst], recv_sem=r_sem.at[src],
            device_id={"sp": dst}, device_id_type=MESH,
        )

    def back_copy(dst, src):
        return pltpu.make_async_remote_copy(
            src_ref=result.at[rows_of(dst, cap)], dst_ref=returned.at[rows_of(src, cap)],
            send_sem=bs_sem.at[dst], recv_sem=br_sem.at[src],
            device_id={"sp": dst}, device_id_type=MESH,
        )

    pl.semaphore_wait(barrier, n)

    @pl.loop(1, n)
    def _(r):
        send_copy(lax.rem(me + r, n), me).start()

    peer = [
        pltpu.make_async_remote_copy(
            src_ref=src.at[0], dst_ref=dst.at[1],
            send_sem=ps_sem.at[i], recv_sem=pr_sem.at[i],
            device_id={"tp": 1 - core}, device_id_type=MESH,
        )
        for i, (src, dst) in enumerate(homes)
    ]
    for copy in peer:
        copy.start()
    arrived[rows_of(me, cap), :] = outbox[rows_of(me, cap), :]
    for copy in local:
        copy.wait()
    for copy in peer:
        copy.wait()

    @pl.loop(1, n)
    def _(r):
        send_copy(me, lax.rem(me + r, n)).wait_recv()

    inner = wg.shape[2]
    tile = 256
    for s in range(2):

        @pl.loop(0, inner // tile)
        def _(j):
            cols = rows_of(j, tile)
            g = dot(arrived[...], wg[s, :, cols])
            u = dot(arrived[...], wu[s, :, cols])
            hidden[s, :, cols] = (g / (1.0 + jnp.exp(-g)) * u).astype(bf16)

    wide = 512

    @pl.loop(0, wd.shape[2] // wide)
    def _(j):
        cols = rows_of(j, wide)
        result[:, cols] = (
            dot(hidden[0], wd[0, :, cols]) + dot(hidden[1], wd[1, :, cols])
        ).astype(bf16)

    @pl.loop(1, n)
    def _(r):
        back_copy(lax.rem(me + r, n), me).start()

    returned[rows_of(me, cap), :] = result[rows_of(me, cap), :]
    high = combine[...].astype(bf16)
    low = (combine[...] - high.astype(f32)).astype(bf16)

    @pl.loop(1, n)
    def _(r):
        back_copy(me, lax.rem(me + r, n)).wait_recv()

    @pl.loop(0, out.shape[1] // wide)
    def _(j):
        cols = rows_of(j, wide)
        back = returned[:, cols]
        out[:, cols] = (
            updated[:, cols].astype(f32) + (dot(high, back) + dot(low, back))
        ).astype(bf16)

    @pl.loop(1, n)
    def _(r):
        dst = lax.rem(me + r, n)
        send_copy(dst, me).wait_send()
        back_copy(dst, me).wait_send()


def solution(mesh):
    n = mesh.shape["sp"]
    vmem = pl.BlockSpec(memory_space=pltpu.VMEM)
    hbm = pl.BlockSpec(memory_space=pl.ANY)
    dma = pltpu.SemaphoreType.DMA

    def body(
        query, forget_logit, value, out_gate, lower_bound, head_gain, residual_in, w_out,
        ffn_gain, routing, route_weight, expert_gate, expert_up, expert_down,
    ):
        length, width = query.shape
        heads = width // HEAD_DIM
        half, model = residual_in.shape
        cap = 2 * half * routing.shape[1] // n
        cap = -(-cap // 16) * 16
        slots = n * cap
        piece = width // n
        updated, outbox, combine = pl.pallas_call(
            functools.partial(scan_kernel, n, cap),
            out_shape=(
                jax.ShapeDtypeStruct((half, model), bf16),
                jax.ShapeDtypeStruct((slots, model), bf16),
                jax.ShapeDtypeStruct((half, slots), f32),
            ),
            in_specs=[vmem] * 10 + [hbm],
            out_specs=(vmem, vmem, vmem),
            scratch_shapes=[
                pltpu.VMEM(w_out.shape, bf16),
                pltpu.VMEM((length, width), bf16),
                pltpu.VMEM((length, width), bf16),
                pltpu.VMEM((length, width), f32),
                pltpu.VMEM((width, HEAD_DIM), bf16),
                pltpu.VMEM((n, piece, HEAD_DIM), bf16),
                pltpu.VMEM((heads, HEAD_DIM), f32),
                pltpu.VMEM((n, heads, HEAD_DIM), f32),
                pltpu.VMEM((n, piece, HEAD_DIM), bf16),
                pltpu.VMEM((width, HEAD_DIM), bf16),
                pltpu.VMEM((2, half, width), bf16),
                pltpu.VMEM((half, width), bf16),
                pltpu.VMEM((half, model), f32),
                dma, dma((n,)), dma((n,)), dma((n,)), dma((n,)), dma((n,)), dma((n,)), dma, dma,
            ],
            compiler_params=pltpu.CompilerParams(
                collective_id=0, has_side_effects=True, vmem_limit_bytes=50 << 20
            ),
        )(
            query, forget_logit, value, out_gate, lower_bound[None], head_gain[None],
            residual_in, ffn_gain[None], routing, route_weight, w_out,
        )
        inner = expert_gate.shape[2]
        return pl.pallas_call(
            functools.partial(expert_kernel, n, cap),
            out_shape=jax.ShapeDtypeStruct((half, model), bf16),
            in_specs=[vmem] * 3 + [hbm] * 3,
            out_specs=vmem,
            scratch_shapes=[
                pltpu.VMEM((2, model, inner), bf16),
                pltpu.VMEM((2, model, inner), bf16),
                pltpu.VMEM((2, inner, model), bf16),
                pltpu.VMEM((slots, model), bf16),
                pltpu.VMEM((2, slots, inner), bf16),
                pltpu.VMEM((slots, model), bf16),
                pltpu.VMEM((slots, model), bf16),
                dma((3,)), dma((3,)), dma((3,)),
                dma((n,)), dma((n,)), dma((n,)), dma((n,)),
            ],
            compiler_params=pltpu.CompilerParams(
                collective_id=1, has_side_effects=True, vmem_limit_bytes=60 << 20
            ),
        )(outbox, updated, combine, expert_gate, expert_up, expert_down)

    placed = (
        P("sp", "tp"), P("sp", "tp"), P("sp", "tp"), P("sp", "tp"), P("tp"), P("tp"),
        P(("sp", "tp"), None), P(), P(), P(("sp", "tp"), None), P(("sp", "tp"), None),
        P("sp", None, "tp"), P("sp", None, "tp"), P("sp", "tp", None),
    )
    return jax.shard_map(
        body, mesh=mesh, in_specs=placed, out_specs=P(("sp", "tp"), None), check_vma=False
    )
```

```python
import functools

import jax
import jax.numpy as jnp
from jax import lax
from jax.experimental import pallas as pl
from jax.experimental.pallas import tpu as pltpu
from jax.sharding import PartitionSpec as P

HEAD_DIM = 128
MESH = pl.DeviceIdType.MESH
epsilon = 1e-06
f32 = jnp.float32
bf16 = jnp.bfloat16
NT = (((1,), (1,)), ((), ()))
TN = (((0,), (0,)), ((), ()))


def dot(a, b, dims=(((1,), (0,)), ((), ())), precision=None):
    return lax.dot_general(a, b, dims, precision=precision, preferred_element_type=f32)


def rows_of(index, count):
    return pl.ds(pl.multiple_of(index * count, count), count)


def greet(n):
    me, core = lax.axis_index("sp"), lax.axis_index("tp")
    barrier = pltpu.get_barrier_semaphore()
    pl.semaphore_signal(barrier, inc=1, device_id={"tp": 1 - core}, device_id_type=MESH)

    @pl.loop(1, n)
    def _(r):
        pl.semaphore_signal(
            barrier, inc=1, device_id={"sp": lax.rem(me + r, n)}, device_id_type=MESH
        )

    return barrier


def partner(me, r):
    other = me
    step = 1
    while step <= r:
        if r & step:
            other = other + step * (1 - 2 * (me // step % 2))
        step *= 2
    return other


def layer_kernel(
    n, cap,
    query_h, logit_h, value_h, gate_h, bound_h, gain_h, residual_h, ffn_gain_h, routing_h,
    weight_h, w_hbm, g_hbm, u_hbm, d_hbm,
    layer_out,
    query, logit, value, gate, bound, gain, residual, ffn_gain, routing, weight,
    w_out, q_scr, k_scr, ho, st_send, st_recv, dec_send, dec_recv, ret_send, ret_recv,
    mixed, regrouped, proj,
    wg, wu, wd, outbox, arrived, hidden, result, returned,
    in_sem, w_sem, s_sem, r_sem, ds_sem, dr_sem, bs_sem, br_sem, ms_sem, mr_sem,
    l_sem, ps_sem, pr_sem, xs_sem, xr_sem, ys_sem, yr_sem,
):
    me, core = lax.axis_index("sp"), lax.axis_index("tp")
    length, width = query.shape
    heads = width // HEAD_DIM
    piece = width // n
    half = length // 2
    moves = [
        pltpu.make_async_copy(src, dst, in_sem.at[i])
        for i, (src, dst) in enumerate((
            (logit_h, logit), (bound_h, bound), (query_h, query), (value_h, value),
            (routing_h, routing), (weight_h, weight), (gate_h, gate), (gain_h, gain),
            (residual_h, residual), (ffn_gain_h, ffn_gain),
        ))
    ]
    for move in moves:
        move.start()
    barrier = greet(n)
    w_copy = pltpu.make_async_copy(w_hbm, w_out, w_sem)
    homes = ((g_hbm, wg), (u_hbm, wu), (d_hbm, wd))
    local = [
        pltpu.make_async_copy(src.at[0], dst.at[0], l_sem.at[i])
        for i, (src, dst) in enumerate(homes)
    ]
    peer = [
        pltpu.make_async_remote_copy(
            src_ref=src.at[0], dst_ref=dst.at[1],
            send_sem=ps_sem.at[i], recv_sem=pr_sem.at[i],
            device_id={"tp": 1 - core}, device_id_type=MESH,
        )
        for i, (src, dst) in enumerate(homes)
    ]
    for move in moves[:4]:
        move.wait()
    w_copy.start()

    row = lax.broadcasted_iota(jnp.int32, (length, length), 0)
    col = lax.broadcasted_iota(jnp.int32, (length, length), 1)
    causal = row >= col
    tri = causal.astype(f32)
    for h in range(heads):
        c = slice(h * HEAD_DIM, (h + 1) * HEAD_DIM)
        key = (1.0 - bound[:, c]) / (1.0 + jnp.exp(logit[:, c].astype(f32)))
        cum = dot(tri, jnp.log1p(-key), precision=lax.Precision.HIGHEST)
        last = cum[length - 1 :, :]
        mid = 0.5 * last
        q_scr[:, c] = (query[:, c].astype(f32) * jnp.exp(cum - mid)).astype(bf16)
        keys = (key * jnp.exp(mid - cum)).astype(bf16)
        k_scr[:, c] = keys
        st_send[c, :] = (dot(value[:, c], keys, TN) * jnp.exp(mid)).astype(bf16)
        dec_send[h : h + 1, :] = last
        if h == (heads - 1) // 2:
            pl.semaphore_wait(barrier, n)
            for copy in peer + local:
                copy.start()

    def state_copy(dst, src):
        return pltpu.make_async_remote_copy(
            src_ref=st_send.at[rows_of(dst, piece)], dst_ref=st_recv.at[src],
            send_sem=s_sem.at[dst], recv_sem=r_sem.at[src],
            device_id={"sp": dst}, device_id_type=MESH,
        )

    def decay_copy(dst, src):
        return pltpu.make_async_remote_copy(
            src_ref=dec_send, dst_ref=dec_recv.at[src],
            send_sem=ds_sem.at[dst], recv_sem=dr_sem.at[src],
            device_id={"sp": dst}, device_id_type=MESH,
        )

    def back_copy(dst, src):
        return pltpu.make_async_remote_copy(
            src_ref=ret_send.at[dst], dst_ref=ret_recv.at[rows_of(src, piece)],
            send_sem=bs_sem.at[dst], recv_sem=br_sem.at[src],
            device_id={"sp": dst}, device_id_type=MESH,
        )

    @pl.loop(1, n)
    def _(r):
        dst = lax.rem(me + r, n)
        decay_copy(dst, me).start()
        state_copy(dst, me).start()

    st_recv[me] = st_send[rows_of(me, piece), :]
    dec_recv[me] = dec_send[...]

    for h in range(heads):
        c = slice(h * HEAD_DIM, (h + 1) * HEAD_DIM)
        scores = jnp.where(causal, dot(q_scr[:, c], k_scr[:, c], NT), 0.0).astype(bf16)
        ho[:, c] = dot(scores, value[:, c])

    slots = n * cap
    for move in moves[4:]:
        move.wait()
    top, count = routing.shape
    eye = lax.broadcasted_iota(jnp.int32, (count, count), 0) == lax.broadcasted_iota(
        jnp.int32, (count, count), 1
    )

    def column(line):
        return jnp.sum(jnp.where(eye, line, 0.0), axis=1, keepdims=True)

    expert = lax.broadcasted_iota(jnp.int32, (count, n), 1).astype(f32)
    slot_of = lax.broadcasted_iota(jnp.int32, (count, slots), 1)
    before = (
        lax.broadcasted_iota(jnp.int32, (count, count), 0)
        > lax.broadcasted_iota(jnp.int32, (count, count), 1)
    ).astype(bf16)
    used = jnp.zeros((1, n), f32)
    picks = jnp.zeros((count, slots), f32)
    combine = jnp.zeros((count, slots), f32)
    for k in range(top):
        hot = (column(routing[k : k + 1, :].astype(f32)) == expert).astype(f32)
        rank = dot(before, hot.astype(bf16)) + used
        used = used + jnp.sum(hot, axis=0, keepdims=True)
        slot = jnp.sum(hot * (rank + expert * cap), axis=1, keepdims=True)
        mine = slot.astype(jnp.int32) == slot_of
        picks = jnp.where(mine, 1.0, picks)
        combine = jnp.where(mine, column(weight[k : k + 1, :]), combine)
    high = combine.astype(bf16)
    both = jnp.concatenate([high, (combine - high.astype(f32)).astype(bf16)], axis=0)

    @pl.loop(1, n)
    def _(r):
        src = lax.rem(me + r, n)
        decay_copy(me, src).wait_recv()
        state_copy(me, src).wait_recv()

    my_head = me * piece // HEAD_DIM

    def prefix(p, acc):
        last = dec_recv[p, pl.ds(my_head, 1), :]
        ret_send[p] = (acc * jnp.exp(0.5 * last)).astype(bf16)
        return acc * jnp.exp(last) + st_recv[p].astype(f32)

    lax.fori_loop(0, n, prefix, jnp.zeros((piece, HEAD_DIM), f32))

    @pl.loop(1, n)
    def _(r):
        back_copy(lax.rem(me + r, n), me).start()

    ret_recv[rows_of(me, piece), :] = ret_send[me]

    @pl.loop(1, n)
    def _(r):
        back_copy(me, lax.rem(me + r, n)).wait_recv()

    for h in range(heads):
        c = slice(h * HEAD_DIM, (h + 1) * HEAD_DIM)
        out = ho[:, c] + dot(q_scr[:, c], ret_recv[c, :], NT)
        out = out * lax.rsqrt(jnp.mean(out * out, axis=1, keepdims=True) + epsilon)
        g = gate[:, c].astype(f32)
        out = (out * gain[:, c] * (g / (1.0 + jnp.exp(-g)))).astype(bf16)
        mixed[0, :, c] = out[:half]
        mixed[1, :, c] = out[half:]

    swap = pltpu.make_async_remote_copy(
        src_ref=mixed.at[1 - core], dst_ref=regrouped,
        send_sem=ms_sem, recv_sem=mr_sem,
        device_id={"tp": 1 - core}, device_id_type=MESH,
    )
    swap.start()
    w_copy.wait()
    tile = 512
    total = w_out.shape[1]

    def project(which, source, first):
        @pl.loop(0, total // tile)
        def _(j):
            cols = pl.ds(pl.multiple_of(j * tile, tile), tile)
            part = dot(source, w_out[rows_of(which, width), cols])
            proj[:, cols] = part if first else proj[:, cols] + part

    project(core, mixed[core], True)
    swap.wait()
    project(1 - core, regrouped[...], False)
    updated = (residual[...].astype(f32) + proj[...]).astype(bf16)
    updated = updated.astype(f32)
    proj[...] = updated
    normed = (
        updated
        * lax.rsqrt(jnp.mean(updated * updated, axis=1, keepdims=True) + epsilon)
        * ffn_gain[...]
    ).astype(bf16)
    outbox[...] = dot(picks.astype(bf16), normed, TN).astype(bf16)

    sets = [
        [r for r in range(n - 1, -1, -1) if (r ^ (r >> 1)) & 1 == which] for which in range(2)
    ]
    place = {r: i for i, r in enumerate(sets[0] + sets[1])}

    def block(r):
        return pl.ds(place[r] * cap, cap)

    def send_copy(r):
        return pltpu.make_async_remote_copy(
            src_ref=outbox.at[rows_of(partner(me, r), cap)], dst_ref=arrived.at[block(r)],
            send_sem=xs_sem.at[r], recv_sem=xr_sem.at[r],
            device_id={"sp": partner(me, r)}, device_id_type=MESH,
        )

    def answer_copy(r):
        return pltpu.make_async_remote_copy(
            src_ref=result.at[block(r)], dst_ref=returned.at[rows_of(me, cap)],
            send_sem=ys_sem.at[r], recv_sem=yr_sem.at[r],
            device_id={"sp": partner(me, r)}, device_id_type=MESH,
        )

    def answer_from(r):
        return pltpu.make_async_remote_copy(
            src_ref=result.at[block(r)], dst_ref=returned.at[rows_of(partner(me, r), cap)],
            send_sem=ys_sem.at[r], recv_sem=yr_sem.at[r],
            device_id={"sp": partner(me, r)}, device_id_type=MESH,
        )

    for r in sets[0] + sets[1]:
        if r:
            send_copy(r).start()
    arrived[block(0), :] = outbox[rows_of(me, cap), :]
    for copy in peer + local:
        copy.wait()
    inner = wg.shape[2]
    narrow = 256
    first = 0
    for group in sets:
        for r in group:
            if r:
                send_copy(r).wait_recv()
        part = slice(first, first + len(group) * cap)
        first = first + len(group) * cap
        for s in range(2):

            @pl.loop(0, inner // narrow)
            def _(j):
                cols = rows_of(j, narrow)
                g = dot(arrived[part, :], wg[s, :, cols])
                u = dot(arrived[part, :], wu[s, :, cols])
                hidden[s, part, cols] = (g / (1.0 + jnp.exp(-g)) * u).astype(bf16)

        @pl.loop(0, total // tile)
        def _(j):
            cols = rows_of(j, tile)
            result[part, cols] = (
                dot(hidden[0, part, :], wd[0, :, cols]) + dot(hidden[1, part, :], wd[1, :, cols])
            ).astype(bf16)

        for r in group:
            if r:
                answer_copy(r).start()

    returned[rows_of(me, cap), :] = result[block(0), :]
    for r in sets[0] + sets[1]:
        if r:
            answer_from(r).wait_recv()

    @pl.loop(0, total // tile)
    def _(j):
        cols = rows_of(j, tile)
        back = dot(both, returned[:, cols])
        layer_out[:, cols] = (proj[:, cols] + (back[:count] + back[count:])).astype(bf16)

    @pl.loop(1, n)
    def _(r):
        dst = lax.rem(me + r, n)
        decay_copy(dst, me).wait_send()
        state_copy(dst, me).wait_send()
        back_copy(dst, me).wait_send()

    for r in range(1, n):
        send_copy(r).wait_send()
        answer_copy(r).wait_send()


def solution(mesh):
    n = mesh.shape["sp"]
    vmem = pl.BlockSpec(memory_space=pltpu.VMEM)
    hbm = pl.BlockSpec(memory_space=pl.ANY)
    dma = pltpu.SemaphoreType.DMA

    def body(
        query, forget_logit, value, out_gate, lower_bound, head_gain, residual_in, w_out,
        ffn_gain, routing, route_weight, expert_gate, expert_up, expert_down,
    ):
        length, width = query.shape
        heads = width // HEAD_DIM
        half, model = residual_in.shape
        cap = 2 * half * routing.shape[1] // n
        cap = -(-cap // 16) * 16
        slots = n * cap
        piece = width // n
        inner = expert_gate.shape[2]
        top = routing.shape[1]
        return pl.pallas_call(
            functools.partial(layer_kernel, n, cap),
            out_shape=jax.ShapeDtypeStruct((half, model), bf16),
            in_specs=[hbm] * 14,
            out_specs=vmem,
            scratch_shapes=[
                pltpu.VMEM((length, width), bf16),
                pltpu.VMEM((length, width), bf16),
                pltpu.VMEM((length, width), bf16),
                pltpu.VMEM((length, width), bf16),
                pltpu.VMEM((1, width), f32),
                pltpu.VMEM((1, width), f32),
                pltpu.VMEM((half, model), bf16),
                pltpu.VMEM((1, model), f32),
                pltpu.VMEM((top, half), jnp.int32),
                pltpu.VMEM((top, half), f32),
                pltpu.VMEM(w_out.shape, bf16),
                pltpu.VMEM((length, width), bf16),
                pltpu.VMEM((length, width), bf16),
                pltpu.VMEM((length, width), f32),
                pltpu.VMEM((width, HEAD_DIM), bf16),
                pltpu.VMEM((n, piece, HEAD_DIM), bf16),
                pltpu.VMEM((heads, HEAD_DIM), f32),
                pltpu.VMEM((n, heads, HEAD_DIM), f32),
                pltpu.VMEM((n, piece, HEAD_DIM), bf16),
                pltpu.VMEM((width, HEAD_DIM), bf16),
                pltpu.VMEM((2, half, width), bf16),
                pltpu.VMEM((half, width), bf16),
                pltpu.VMEM((half, model), f32),
                pltpu.VMEM((2, model, inner), bf16),
                pltpu.VMEM((2, model, inner), bf16),
                pltpu.VMEM((2, inner, model), bf16),
                pltpu.VMEM((slots, model), bf16),
                pltpu.VMEM((slots, model), bf16),
                pltpu.VMEM((2, slots, inner), bf16),
                pltpu.VMEM((slots, model), bf16),
                pltpu.VMEM((slots, model), bf16),
                dma((10,)), dma, dma((n,)), dma((n,)), dma((n,)), dma((n,)), dma((n,)), dma((n,)),
                dma, dma, dma((3,)), dma((3,)), dma((3,)),
                dma((n,)), dma((n,)), dma((n,)), dma((n,)),
            ],
            compiler_params=pltpu.CompilerParams(
                collective_id=0, has_side_effects=True, vmem_limit_bytes=60 << 20
            ),
        )(
            query, forget_logit, value, out_gate, lower_bound[None], head_gain[None],
            residual_in, ffn_gain[None], routing.T, route_weight.T, w_out,
            expert_gate, expert_up, expert_down,
        )

    placed = (
        P("sp", "tp"), P("sp", "tp"), P("sp", "tp"), P("sp", "tp"), P("tp"), P("tp"),
        P(("sp", "tp"), None), P(), P(), P(("sp", "tp"), None), P(("sp", "tp"), None),
        P("sp", None, "tp"), P("sp", None, "tp"), P("sp", "tp", None),
    )
    return jax.shard_map(
        body, mesh=mesh, in_specs=placed, out_specs=P(("sp", "tp"), None), check_vma=False
    )
```

```python
import functools

import jax
import jax.numpy as jnp
from jax import lax
from jax.experimental import pallas as pl
from jax.experimental.pallas import tpu as pltpu
from jax.sharding import PartitionSpec as P

HEAD_DIM = 128
MESH = pl.DeviceIdType.MESH
epsilon = 1e-06
f32 = jnp.float32
bf16 = jnp.bfloat16
NT = (((1,), (1,)), ((), ()))
TN = (((0,), (0,)), ((), ()))


def dot(a, b, dims=(((1,), (0,)), ((), ())), precision=None):
    return lax.dot_general(a, b, dims, precision=precision, preferred_element_type=f32)


def rows_of(index, count):
    return pl.ds(pl.multiple_of(index * count, count), count)


def greet(n):
    me, core = lax.axis_index("sp"), lax.axis_index("tp")
    barrier = pltpu.get_barrier_semaphore()
    pl.semaphore_signal(barrier, inc=1, device_id={"tp": 1 - core}, device_id_type=MESH)

    @pl.loop(1, n)
    def _(r):
        pl.semaphore_signal(
            barrier, inc=1, device_id={"sp": lax.rem(me + r, n)}, device_id_type=MESH
        )

    return barrier


def partner(me, r):
    other = me
    step = 1
    while step <= r:
        if r & step:
            other = other + step * (1 - 2 * (me // step % 2))
        step *= 2
    return other


def layer_kernel(
    n, cap,
    query_h, logit_h, value_h, gate_h, bound_h, gain_h, residual_h, ffn_gain_h, routing_h,
    weight_h, w_hbm, g_hbm, u_hbm, d_hbm,
    layer_out,
    query, logit, value, gate, bound, gain, residual, ffn_gain, routing, weight,
    w_out, q_scr, k_scr, ho, st_send, st_recv, dec_send, dec_recv, ret_send, ret_recv,
    mixed, regrouped, proj,
    wg, wu, wd, outbox, arrived, hidden, result, returned,
    in_sem, w_sem, s_sem, r_sem, ds_sem, dr_sem, bs_sem, br_sem, ms_sem, mr_sem,
    l_sem, ps_sem, pr_sem, xs_sem, xr_sem, ys_sem, yr_sem,
):
    me, core = lax.axis_index("sp"), lax.axis_index("tp")
    length, width = query.shape
    heads = width // HEAD_DIM
    groups, piece = st_recv.shape[0], st_recv.shape[2]
    per = heads // groups
    half = length // 2
    moves = [
        pltpu.make_async_copy(src, dst, in_sem.at[i])
        for i, (src, dst) in enumerate((
            (logit_h, logit), (bound_h, bound), (query_h, query), (value_h, value),
            (routing_h, routing), (weight_h, weight), (gate_h, gate), (gain_h, gain),
            (residual_h, residual), (ffn_gain_h, ffn_gain),
        ))
    ]
    for move in moves:
        move.start()
    barrier = greet(n)
    w_copy = pltpu.make_async_copy(w_hbm, w_out, w_sem)
    homes = ((g_hbm, wg), (u_hbm, wu), (d_hbm, wd))
    local = [
        pltpu.make_async_copy(src.at[0], dst.at[0], l_sem.at[i])
        for i, (src, dst) in enumerate(homes)
    ]
    peer = [
        pltpu.make_async_remote_copy(
            src_ref=src.at[0], dst_ref=dst.at[1],
            send_sem=ps_sem.at[i], recv_sem=pr_sem.at[i],
            device_id={"tp": 1 - core}, device_id_type=MESH,
        )
        for i, (src, dst) in enumerate(homes)
    ]
    for move in moves[:4]:
        move.wait()
    w_copy.start()

    row = lax.broadcasted_iota(jnp.int32, (length, length), 0)
    col = lax.broadcasted_iota(jnp.int32, (length, length), 1)
    causal = row >= col
    tri = causal.astype(f32)
    def owned(g, index):
        return pl.ds(pl.multiple_of(g * per * HEAD_DIM + index * piece, piece), piece)

    def state_copy(g, r):
        return pltpu.make_async_remote_copy(
            src_ref=st_send.at[owned(g, partner(me, r))], dst_ref=st_recv.at[g, r],
            send_sem=s_sem.at[g, r], recv_sem=r_sem.at[g, r],
            device_id={"sp": partner(me, r)}, device_id_type=MESH,
        )

    def decay_copy(g, r):
        return pltpu.make_async_remote_copy(
            src_ref=dec_send.at[g], dst_ref=dec_recv.at[g, r],
            send_sem=ds_sem.at[g, r], recv_sem=dr_sem.at[g, r],
            device_id={"sp": partner(me, r)}, device_id_type=MESH,
        )

    def back_copy(g, r):
        return pltpu.make_async_remote_copy(
            src_ref=ret_send.at[g, partner(me, r)], dst_ref=ret_recv.at[owned(g, me)],
            send_sem=bs_sem.at[g, r], recv_sem=br_sem.at[g, r],
            device_id={"sp": partner(me, r)}, device_id_type=MESH,
        )

    def back_from(g, r):
        return pltpu.make_async_remote_copy(
            src_ref=ret_send.at[g, me], dst_ref=ret_recv.at[owned(g, partner(me, r))],
            send_sem=bs_sem.at[g, r], recv_sem=br_sem.at[g, r],
            device_id={"sp": partner(me, r)}, device_id_type=MESH,
        )

    others = range(n - 1, 0, -1)

    for h in range(heads):
        c = slice(h * HEAD_DIM, (h + 1) * HEAD_DIM)
        key = (1.0 - bound[:, c]) / (1.0 + jnp.exp(logit[:, c].astype(f32)))
        cum = dot(tri, jnp.log1p(-key), precision=lax.Precision.HIGHEST)
        last = cum[length - 1 :, :]
        mid = 0.5 * last
        q_scr[:, c] = (query[:, c].astype(f32) * jnp.exp(cum - mid)).astype(bf16)
        keys = (key * jnp.exp(mid - cum)).astype(bf16)
        k_scr[:, c] = keys
        st_send[c, :] = (dot(value[:, c], keys, TN) * jnp.exp(mid)).astype(bf16)
        g = h // per
        dec_send[g, h % per : h % per + 1, :] = last
        if h == 0:
            pl.semaphore_wait(barrier, n)
        if h % per == per - 1:
            for r in others:
                decay_copy(g, r).start()
                state_copy(g, r).start()
            st_recv[g, 0] = st_send[owned(g, me), :]
            dec_recv[g, 0] = dec_send[g]
            if g == 0:
                for copy in peer + local:
                    copy.start()

    for h in range(heads):
        c = slice(h * HEAD_DIM, (h + 1) * HEAD_DIM)
        scores = jnp.where(causal, dot(q_scr[:, c], k_scr[:, c], NT), 0.0).astype(bf16)
        ho[:, c] = dot(scores, value[:, c])

    slots = n * cap
    for move in moves[4:]:
        move.wait()
    top, count = routing.shape
    eye = lax.broadcasted_iota(jnp.int32, (count, count), 0) == lax.broadcasted_iota(
        jnp.int32, (count, count), 1
    )

    def column(line):
        return jnp.sum(jnp.where(eye, line, 0.0), axis=1, keepdims=True)

    expert = lax.broadcasted_iota(jnp.int32, (count, n), 1).astype(f32)
    slot_of = lax.broadcasted_iota(jnp.int32, (count, slots), 1)
    before = (
        lax.broadcasted_iota(jnp.int32, (count, count), 0)
        > lax.broadcasted_iota(jnp.int32, (count, count), 1)
    ).astype(bf16)
    used = jnp.zeros((1, n), f32)
    picks = jnp.zeros((count, slots), f32)
    combine = jnp.zeros((count, slots), f32)
    for k in range(top):
        hot = (column(routing[k : k + 1, :].astype(f32)) == expert).astype(f32)
        rank = dot(before, hot.astype(bf16)) + used
        used = used + jnp.sum(hot, axis=0, keepdims=True)
        slot = jnp.sum(hot * (rank + expert * cap), axis=1, keepdims=True)
        mine = slot.astype(jnp.int32) == slot_of
        picks = jnp.where(mine, 1.0, picks)
        combine = jnp.where(mine, column(weight[k : k + 1, :]), combine)
    high = combine.astype(bf16)
    both = jnp.concatenate([high, (combine - high.astype(f32)).astype(bf16)], axis=0)

    for g in range(groups):
        for r in others:
            decay_copy(g, r).wait_recv()
            state_copy(g, r).wait_recv()
        own_head = me * piece // HEAD_DIM

        def prefix(p, acc):
            r = 0
            step = 1
            while step < n:
                r = r + step * ((me // step + p // step) % 2)
                step *= 2
            last = dec_recv[g, r, pl.ds(own_head, 1), :]
            ret_send[g, p] = (acc * jnp.exp(0.5 * last)).astype(bf16)
            return acc * jnp.exp(last) + st_recv[g, r].astype(f32)

        lax.fori_loop(0, n, prefix, jnp.zeros((piece, HEAD_DIM), f32))
        for r in others:
            back_copy(g, r).start()
        ret_recv[owned(g, me), :] = ret_send[g, me]

    for h in range(heads):
        c = slice(h * HEAD_DIM, (h + 1) * HEAD_DIM)
        if h % per == 0:
            for r in others:
                back_from(h // per, r).wait_recv()
        out = ho[:, c] + dot(q_scr[:, c], ret_recv[c, :], NT)
        out = out * lax.rsqrt(jnp.mean(out * out, axis=1, keepdims=True) + epsilon)
        g = gate[:, c].astype(f32)
        out = (out * gain[:, c] * (g / (1.0 + jnp.exp(-g)))).astype(bf16)
        mixed[0, :, c] = out[:half]
        mixed[1, :, c] = out[half:]

    swap = pltpu.make_async_remote_copy(
        src_ref=mixed.at[1 - core], dst_ref=regrouped,
        send_sem=ms_sem, recv_sem=mr_sem,
        device_id={"tp": 1 - core}, device_id_type=MESH,
    )
    swap.start()
    w_copy.wait()
    tile = 512
    total = w_out.shape[1]

    def project(which, source, first):
        @pl.loop(0, total // tile)
        def _(j):
            cols = pl.ds(pl.multiple_of(j * tile, tile), tile)
            part = dot(source, w_out[rows_of(which, width), cols])
            proj[:, cols] = part if first else proj[:, cols] + part

    project(core, mixed[core], True)
    swap.wait()
    project(1 - core, regrouped[...], False)
    updated = (residual[...].astype(f32) + proj[...]).astype(bf16)
    updated = updated.astype(f32)
    proj[...] = updated
    normed = (
        updated
        * lax.rsqrt(jnp.mean(updated * updated, axis=1, keepdims=True) + epsilon)
        * ffn_gain[...]
    ).astype(bf16)
    outbox[...] = dot(picks.astype(bf16), normed, TN).astype(bf16)

    sets = [
        [r for r in range(n - 1, -1, -1) if (r ^ (r >> 1)) & 1 == which] for which in range(2)
    ]
    place = {r: i for i, r in enumerate(sets[0] + sets[1])}

    def block(r):
        return pl.ds(place[r] * cap, cap)

    def send_copy(r):
        return pltpu.make_async_remote_copy(
            src_ref=outbox.at[rows_of(partner(me, r), cap)], dst_ref=arrived.at[block(r)],
            send_sem=xs_sem.at[r], recv_sem=xr_sem.at[r],
            device_id={"sp": partner(me, r)}, device_id_type=MESH,
        )

    def answer_copy(r):
        return pltpu.make_async_remote_copy(
            src_ref=result.at[block(r)], dst_ref=returned.at[rows_of(me, cap)],
            send_sem=ys_sem.at[r], recv_sem=yr_sem.at[r],
            device_id={"sp": partner(me, r)}, device_id_type=MESH,
        )

    def answer_from(r):
        return pltpu.make_async_remote_copy(
            src_ref=result.at[block(r)], dst_ref=returned.at[rows_of(partner(me, r), cap)],
            send_sem=ys_sem.at[r], recv_sem=yr_sem.at[r],
            device_id={"sp": partner(me, r)}, device_id_type=MESH,
        )

    for r in sets[0] + sets[1]:
        if r:
            send_copy(r).start()
    arrived[block(0), :] = outbox[rows_of(me, cap), :]
    for copy in peer + local:
        copy.wait()
    inner = wg.shape[2]
    narrow = 256
    first = 0
    for group in sets:
        for r in group:
            if r:
                send_copy(r).wait_recv()
        part = slice(first, first + len(group) * cap)
        first = first + len(group) * cap
        for s in range(2):

            @pl.loop(0, inner // narrow)
            def _(j):
                cols = rows_of(j, narrow)
                g = dot(arrived[part, :], wg[s, :, cols])
                u = dot(arrived[part, :], wu[s, :, cols])
                hidden[s, part, cols] = (g / (1.0 + jnp.exp(-g)) * u).astype(bf16)

        @pl.loop(0, total // tile)
        def _(j):
            cols = rows_of(j, tile)
            result[part, cols] = (
                dot(hidden[0, part, :], wd[0, :, cols]) + dot(hidden[1, part, :], wd[1, :, cols])
            ).astype(bf16)

        for r in group:
            if r:
                answer_copy(r).start()

    returned[rows_of(me, cap), :] = result[block(0), :]
    for r in sets[0] + sets[1]:
        if r:
            answer_from(r).wait_recv()

    @pl.loop(0, total // tile)
    def _(j):
        cols = rows_of(j, tile)
        back = dot(both, returned[:, cols])
        layer_out[:, cols] = (proj[:, cols] + (back[:count] + back[count:])).astype(bf16)

    for g in range(groups):
        for r in others:
            decay_copy(g, r).wait_send()
            state_copy(g, r).wait_send()
            back_copy(g, r).wait_send()

    for r in range(1, n):
        send_copy(r).wait_send()
        answer_copy(r).wait_send()


def solution(mesh):
    n = mesh.shape["sp"]
    vmem = pl.BlockSpec(memory_space=pltpu.VMEM)
    hbm = pl.BlockSpec(memory_space=pl.ANY)
    dma = pltpu.SemaphoreType.DMA

    def body(
        query, forget_logit, value, out_gate, lower_bound, head_gain, residual_in, w_out,
        ffn_gain, routing, route_weight, expert_gate, expert_up, expert_down,
    ):
        length, width = query.shape
        heads = width // HEAD_DIM
        half, model = residual_in.shape
        cap = 2 * half * routing.shape[1] // n
        cap = -(-cap // 16) * 16
        slots = n * cap
        groups = 2 if heads % 2 == 0 and width // n % 32 == 0 else 1
        piece = width // n // groups
        inner = expert_gate.shape[2]
        top = routing.shape[1]
        return pl.pallas_call(
            functools.partial(layer_kernel, n, cap),
            out_shape=jax.ShapeDtypeStruct((half, model), bf16),
            in_specs=[hbm] * 14,
            out_specs=vmem,
            scratch_shapes=[
                pltpu.VMEM((length, width), bf16),
                pltpu.VMEM((length, width), bf16),
                pltpu.VMEM((length, width), bf16),
                pltpu.VMEM((length, width), bf16),
                pltpu.VMEM((1, width), f32),
                pltpu.VMEM((1, width), f32),
                pltpu.VMEM((half, model), bf16),
                pltpu.VMEM((1, model), f32),
                pltpu.VMEM((top, half), jnp.int32),
                pltpu.VMEM((top, half), f32),
                pltpu.VMEM(w_out.shape, bf16),
                pltpu.VMEM((length, width), bf16),
                pltpu.VMEM((length, width), bf16),
                pltpu.VMEM((length, width), f32),
                pltpu.VMEM((width, HEAD_DIM), bf16),
                pltpu.VMEM((groups, n, piece, HEAD_DIM), bf16),
                pltpu.VMEM((groups, heads // groups, HEAD_DIM), f32),
                pltpu.VMEM((groups, n, heads // groups, HEAD_DIM), f32),
                pltpu.VMEM((groups, n, piece, HEAD_DIM), bf16),
                pltpu.VMEM((width, HEAD_DIM), bf16),
                pltpu.VMEM((2, half, width), bf16),
                pltpu.VMEM((half, width), bf16),
                pltpu.VMEM((half, model), f32),
                pltpu.VMEM((2, model, inner), bf16),
                pltpu.VMEM((2, model, inner), bf16),
                pltpu.VMEM((2, inner, model), bf16),
                pltpu.VMEM((slots, model), bf16),
                pltpu.VMEM((slots, model), bf16),
                pltpu.VMEM((2, slots, inner), bf16),
                pltpu.VMEM((slots, model), bf16),
                pltpu.VMEM((slots, model), bf16),
                dma((10,)), dma,
                dma((groups, n)), dma((groups, n)), dma((groups, n)),
                dma((groups, n)), dma((groups, n)), dma((groups, n)),
                dma, dma, dma((3,)), dma((3,)), dma((3,)),
                dma((n,)), dma((n,)), dma((n,)), dma((n,)),
            ],
            compiler_params=pltpu.CompilerParams(
                collective_id=0, has_side_effects=True, vmem_limit_bytes=60 << 20
            ),
        )(
            query, forget_logit, value, out_gate, lower_bound[None], head_gain[None],
            residual_in, ffn_gain[None], routing.T, route_weight.T, w_out,
            expert_gate, expert_up, expert_down,
        )

    placed = (
        P("sp", "tp"), P("sp", "tp"), P("sp", "tp"), P("sp", "tp"), P("tp"), P("tp"),
        P(("sp", "tp"), None), P(), P(), P(("sp", "tp"), None), P(("sp", "tp"), None),
        P("sp", None, "tp"), P("sp", None, "tp"), P("sp", "tp", None),
    )
    return jax.shard_map(
        body, mesh=mesh, in_specs=placed, out_specs=P(("sp", "tp"), None), check_vma=False
    )
```
